32 devices in a mesh: rep: 2 (over x), fs: 4 (over z), tp: 4 (over y, core).
Axes of the slice: x: 2, y: 2, z: 4, core: 2. Of those that a mesh axis runs over, the one named last changes fastest.
Arguments:
- tokens: bfloat16 [4096, 2048], P(('rep', 'fs', 'tp')), may hold values from -6 to 6
- mix_gain: bfloat16 [2048], replicated, may hold values from 0.099609375 to 1.8984375
- gate_proj: bfloat16 [2048, 512], P('fs', 'tp'), may hold values from -0.125 to 0.125
- value_proj: bfloat16 [2048, 512], P('fs', 'tp'), may hold values from -1 to 1
- layer_gain: bfloat16 [512], replicated, may hold values from 0.099609375 to 1.8984375
- layer_shift: bfloat16 [512], replicated, may hold values from -3 to 3
- mix_kernel: bfloat16 [4, 128, 128], replicated, may hold values from -0.5 to 0.5
- mix_offset: bfloat16 [4, 128], replicated, may hold values from -4 to 4
- out_proj: bfloat16 [2048, 512], P('fs', 'tp'), may hold values from -0.25 to 0.25
- ffn_gain: bfloat16 [2048], replicated, may hold values from 0.099609375 to 1.8984375
- ffn_gate: bfloat16 [2048, 5632], P('fs', 'tp'), may hold values from -0.125 to 0.125
- ffn_up: bfloat16 [2048, 5632], P('fs', 'tp'), may hold values from -0.125 to 0.125
- ffn_down: bfloat16 [2048, 5632], P('fs', 'tp'), may hold values from -0.078125 to 0.078125
Outputs:
- layer_out: bfloat16 [4096, 2048], P(('rep', 'fs', 'tp'))
The draws below stay inside these ranges and needn't reach their ends.
All inputs are finite; a program needn't handle non-finite values.
Results may differ from the reference program's by a relative error of at most 0.015.
Values may be sent and summed in bfloat16 or wider, within the bound.
A program may use at most 64 MiB of HBM per device.

```python
import math
import jax
import jax.numpy as jnp
from jax import lax

D = 2048
FF = 5632
W = 512
GROUP_CH = 128
BLOCK = 128
GROUPS = 4
TOKENS = 4096
N_TP = 4


def draw_value_proj(key, part):
    key_entries = jax.random.fold_in(key, 11)
    key_columns = jax.random.fold_in(key, 12)
    column_pos = jnp.arange(W, dtype=jnp.float32) / max(W - 1, 1)
    jitter = jnp.exp(jax.random.uniform(key_columns, (W,), jnp.float32, 0.0, math.log(4.0)))
    entries = jax.random.normal(key_entries, (D, W), jnp.float32)
    trend = jnp.exp(column_pos * math.log(3.0))
    scaled = entries * D ** (-0.5) * trend[None, :] * jitter[None, :]
    return jnp.clip(scaled, -1.0, 1.0).astype(jnp.bfloat16)


def block_levels(key, dims, pieces, least, high):
    def one(axis_at, shards_of):
        steps = jax.random.uniform(jax.random.fold_in(jax.random.fold_in(key, 6), axis_at), (shards_of,), jnp.float32, least / len(pieces), high / len(pieces))
        return jnp.repeat(jnp.exp(steps), dims[axis_at] // shards_of).reshape((-1,) + (1,) * (len(dims) - axis_at - 1))

    loudness = one(*pieces[0])
    for cut in pieces[1:]:
        loudness = loudness * one(*cut)
    return loudness


def normal_values(rng, dims, width, limit, pieces=(), kind=jnp.bfloat16):
    values = width * jax.random.normal(rng, dims, jnp.float32)
    if pieces:
        values = values * block_levels(rng, dims, pieces, -0.22, 0.18)
    return jnp.clip(values, -limit, limit).astype(kind)


def setup_inputs(seed: int = 0) -> dict:
    streams_of = jax.random.split(jax.random.key(seed), 14)
    tokens = normal_values(streams_of[0], (TOKENS, D), 1.0, 6.0, ((0, 32),))
    mix_gain = jnp.clip(1.0 + 0.18 * jax.random.normal(streams_of[1], (D,), jnp.float32), 0.099609375, 1.8984375).astype(jnp.bfloat16)
    gate_proj = normal_values(streams_of[2], (D, W), D ** -0.5, 0.125, ((0, 4), (1, 4)))
    value_proj = draw_value_proj(jax.random.fold_in(streams_of[13], 71), 0)
    layer_gain = jnp.clip(1.0 + 0.18 * jax.random.normal(streams_of[4], (W,), jnp.float32), 0.099609375, 1.8984375).astype(jnp.bfloat16)
    layer_shift = normal_values(streams_of[5], (W,), 0.5, 3.0)
    mix_kernel = normal_values(streams_of[6], (GROUPS, BLOCK, BLOCK), BLOCK ** -0.5, 0.5)
    mix_offset = normal_values(streams_of[7], (GROUPS, BLOCK), 1.0, 4.0)
    out_proj = normal_values(streams_of[8], (D, W), W ** -0.5, 0.25, ((0, 4), (1, 4)))
    ffn_gain = jnp.clip(1.0 + 0.18 * jax.random.normal(streams_of[9], (D,), jnp.float32), 0.099609375, 1.8984375).astype(jnp.bfloat16)
    ffn_gate = normal_values(streams_of[10], (D, FF), D ** -0.5, 0.125, ((0, 4), (1, 4)))
    ffn_up = normal_values(streams_of[11], (D, FF), D ** -0.5, 0.125, ((0, 4), (1, 4)))
    ffn_down = normal_values(streams_of[12], (D, FF), FF ** -0.5, 0.078125, ((0, 4), (1, 4)))
    return dict(tokens=tokens, mix_gain=mix_gain, gate_proj=gate_proj, value_proj=value_proj, layer_gain=layer_gain, layer_shift=layer_shift, mix_kernel=mix_kernel, mix_offset=mix_offset, out_proj=out_proj, ffn_gain=ffn_gain, ffn_gate=ffn_gate, ffn_up=ffn_up, ffn_down=ffn_down)


epsilon = 1e-06

def rms_norm(rows, gain):
    floats = rows.astype(jnp.float32)
    scale = lax.rsqrt(lax.optimization_barrier(jnp.mean(floats * floats, axis=-1, keepdims=True)) + epsilon)
    return (floats * scale * gain.astype(jnp.float32)).astype(jnp.bfloat16)

def reference(tokens, mix_gain, gate_proj, value_proj, layer_gain, layer_shift, mix_kernel, mix_offset, out_proj, ffn_gain, ffn_gate, ffn_up, ffn_down):
    normed = rms_norm(tokens, mix_gain)
    gate_u = jax.nn.gelu(jnp.dot(normed, gate_proj, preferred_element_type=jnp.float32))
    activated = jax.nn.gelu(jnp.dot(normed, value_proj, preferred_element_type=jnp.float32))
    center = lax.optimization_barrier(jnp.sum(activated, axis=-1, keepdims=True)) / W
    spread = lax.optimization_barrier(jnp.sum(activated * activated, axis=-1, keepdims=True)) / W - center * center
    values = ((activated - center) * lax.rsqrt(spread + epsilon) * layer_gain.astype(jnp.float32) + layer_shift.astype(jnp.float32)).astype(jnp.bfloat16)
    causal = jnp.tril(jnp.ones((BLOCK, BLOCK), dtype=bool))
    masked = jnp.where(causal[None], mix_kernel, jnp.zeros_like(mix_kernel))
    blocks = values.reshape(-1, BLOCK, GROUPS, GROUP_CH).astype(jnp.float32)
    mixing = jnp.einsum('gts,nsgc->ntgc', masked.astype(jnp.float32), blocks)
    mixing = mixing + mix_offset.astype(jnp.float32).T[None, :, :, None]
    gated_rows = (gate_u * mixing.reshape(gate_u.shape)).astype(jnp.bfloat16)
    mixer_out = lax.dot_general(gated_rows, out_proj, (((1,), (1,)), ((), ())), preferred_element_type=jnp.float32)
    middle = (tokens.astype(jnp.float32) + mixer_out).astype(jnp.bfloat16)
    normed2 = rms_norm(middle, ffn_gain)
    gate_pre = jnp.dot(normed2, ffn_gate, preferred_element_type=jnp.float32)
    up_pre = jnp.dot(normed2, ffn_up, preferred_element_type=jnp.float32)
    hidden = (jax.nn.silu(gate_pre) * up_pre).astype(jnp.bfloat16)
    run_len = FF // N_TP
    summed = jnp.zeros((tokens.shape[0], D), jnp.float32)
    for run_id in range(N_TP):
        hidden_run = hidden[:, run_id * run_len:(run_id + 1) * run_len]
        weight_run = ffn_down[:, run_id * run_len:(run_id + 1) * run_len]
        partial_value = lax.dot_general(hidden_run, weight_run, (((1,), (1,)), ((), ())), preferred_element_type=jnp.float32)
        summed = summed + partial_value.astype(jnp.bfloat16).astype(jnp.float32)
    return (middle.astype(jnp.float32) + summed).astype(jnp.bfloat16)
```

```python
import functools

import jax
import jax.numpy as jnp
from jax import lax
from jax.experimental import pallas as pl
from jax.experimental.pallas import tpu as pltpu
from jax.sharding import PartitionSpec as P

epsilon = 1e-06
MESH = pl.DeviceIdType.MESH
F32 = jnp.float32
BF16 = jnp.bfloat16


def rms_norm(floats, gain):
    scale = lax.rsqrt(jnp.mean(floats * floats, axis=-1, keepdims=True) + epsilon)
    return (floats * scale * gain).astype(BF16)


def gelu(x):
    inner = 0.7978845608028654 * (x + 0.044715 * (x * x * x))
    return 0.5 * x * (1.0 + jnp.tanh(inner))


def contract_last(left, right):
    return lax.dot_general(left, right, (((1,), (1,)), ((), ())), preferred_element_type=F32)


def kernel(
    sizes,
    tok_ref,
    mg_ref,
    lg_ref,
    ls_ref,
    mk_ref,
    mo_ref,
    fg_ref,
    m_ref,
    g_ref,
    d_ref,
    out_ref,
    mbuf,
    gbuf,
    dbuf,
    nall,
    gate_u,
    act,
    stats,
    obuf,
    orecv,
    mid,
    xall,
    hbuf,
    pbuf,
    prow,
    ring_s,
    ring_r,
    n_s,
    n_r,
    st_s,
    st_r,
    o_s,
    o_r,
    x_s,
    x_r,
    p_s,
    p_r,
):
    n_rep, n_fs, n_tp, width, lw, lwp, group_ch, half = sizes
    tok, model = tok_ref.shape
    depth = m_ref.shape[0]
    part = depth // 2
    rep, fs, tp = lax.axis_index("rep"), lax.axis_index("fs"), lax.axis_index("tp")
    n_g = n_rep * n_tp
    g_id = rep * n_tp + tp
    right = lax.rem(fs + 1, n_fs)
    left = lax.rem(fs + n_fs - 1, n_fs)

    def group_peer(d):
        other = lax.rem(g_id + d, n_g)
        return other, {"rep": other // n_tp, "tp": lax.rem(other, n_tp)}

    def tp_peer(d):
        other = lax.rem(tp + d, n_tp)
        return other, {"tp": other}

    barrier = pltpu.get_barrier_semaphore()
    for side in (left, right):
        pl.semaphore_signal(barrier, inc=1, device_id={"fs": side}, device_id_type=MESH)
    for d in range(1, n_g):
        pl.semaphore_signal(barrier, inc=1, device_id=group_peer(d)[1], device_id_type=MESH)
    pl.semaphore_wait(barrier, n_g + 1)

    held = ((m_ref, mbuf), (g_ref, gbuf), (d_ref, dbuf))

    def block(p, s):
        return held[p][0] if s == 0 else held[p][1].at[s - 1]

    def ring(p, h, s):
        rows = pl.ds(h * part, part)
        return pltpu.make_async_remote_copy(
            src_ref=block(p, s - 1).at[rows],
            dst_ref=block(p, s).at[rows],
            send_sem=ring_s.at[p, h, s - 1],
            recv_sem=ring_r.at[p, h, s - 1],
            device_id={"fs": right},
            device_id_type=MESH,
        )

    def columns(s, size=None):
        size = depth if size is None else size
        owner = lax.rem(fs - s + n_fs, n_fs)
        return pl.multiple_of(owner * depth, 128)

    ring(0, 0, 1).start()
    ring(0, 1, 1).start()

    nmine = pl.ds(pl.multiple_of(tp * tok, tok), tok)
    nall[nmine, :] = rms_norm(tok_ref[...].astype(F32), mg_ref[...].astype(F32))

    def ncopy(d):
        return pltpu.make_async_remote_copy(
            src_ref=nall.at[nmine],
            dst_ref=nall.at[nmine],
            send_sem=n_s.at[d - 1],
            recv_sem=n_r.at[d - 1],
            device_id=tp_peer(d)[1],
            device_id_type=MESH,
        )

    for d in range(1, n_tp):
        ncopy(d).start()
    for s in range(2, n_fs):
        for h in range(2):
            ring(0, h, s - 1).wait_recv()
            ring(0, h, s).start()
    ring(1, 0, 1).start()
    ring(1, 1, 1).start()
    for h in range(2):
        ring(0, h, n_fs - 1).wait_recv()
    for d in range(1, n_tp):
        ncopy(d).wait_recv()

    rows_tp = n_tp * tok

    def project(i, carry):
        rows = pl.ds(pl.multiple_of(i * tok, tok), tok)
        pre = jnp.zeros((tok, 2 * lwp), F32)
        for s in range(n_fs):
            pre = pre + jnp.dot(
                nall[rows, pl.ds(columns(s), depth)],
                block(0, s)[:, : 2 * lwp],
                preferred_element_type=F32,
            )
        gate_u[rows, :] = gelu(pre[:, :lwp])
        a = gelu(pre[:, lwp:])
        act[rows, :] = a
        flipped = a.T
        one = jnp.sum(flipped, axis=0, keepdims=True)
        two = jnp.sum(flipped * flipped, axis=0, keepdims=True)
        which = lax.broadcasted_iota(jnp.int32, (8, tok), 0)
        stats[0, i] = jnp.where(which == 0, one, two)
        return carry

    lax.fori_loop(0, n_tp, project, 0)

    def stcopy(d):
        return pltpu.make_async_remote_copy(
            src_ref=stats.at[0],
            dst_ref=stats.at[d],
            send_sem=st_s.at[d - 1],
            recv_sem=st_r.at[d - 1],
            device_id=tp_peer(d)[1],
            device_id_type=MESH,
        )

    for d in range(1, n_tp):
        stcopy(d).start()
    for d in range(1, n_tp):
        stcopy(d).wait_recv()

    group = (tp * lw) // group_ch
    span = mk_ref.shape[1]
    at_t = lax.broadcasted_iota(jnp.int32, (span, span), 0)
    at_s = lax.broadcasted_iota(jnp.int32, (span, span), 1)
    mix_k = jnp.where(at_s <= at_t, mk_ref[group].astype(F32), 0.0).astype(BF16)
    gain_part, shift_part, offset = lg_ref[tp], ls_ref[tp], mo_ref[group]

    def mix(i, carry):
        rows = pl.ds(pl.multiple_of(i * tok, tok), tok)
        total = stats[0, i]
        for d in range(1, n_tp):
            total = total + stats[d, i]
        flipped = jnp.concatenate([total] * 16, axis=0).T
        center = flipped[:, 0:1] / width
        spread = flipped[:, 1:2] / width - center * center
        values = (
            (act[rows, :] - center) * lax.rsqrt(spread + epsilon) * gain_part + shift_part
        ).astype(BF16)
        gates = gate_u[rows, :]
        for b in range(tok // span):
            cut = slice(b * span, (b + 1) * span)
            mixing = jnp.dot(mix_k, values[cut], preferred_element_type=F32) + offset
            gated = (gates[cut] * mixing).astype(BF16)
            to = pl.ds(pl.multiple_of(i * tok + b * span, span), span)
            for s in range(n_fs):
                obuf[to, pl.ds(columns(s), depth)] = contract_last(
                    gated, block(0, s)[:, 2 * lwp :]
                ).astype(BF16)
        return carry

    lax.fori_loop(0, n_tp, mix, 0)

    def ocopy(d):
        other, where = tp_peer(d)
        return pltpu.make_async_remote_copy(
            src_ref=obuf.at[pl.ds(pl.multiple_of(other * tok, tok), tok)],
            dst_ref=orecv.at[d - 1],
            send_sem=o_s.at[d - 1],
            recv_sem=o_r.at[d - 1],
            device_id=where,
            device_id_type=MESH,
        )

    for d in range(1, n_tp):
        ocopy(d).start()

    steps = [(h, s) for s in range(2, n_fs) for h in range(2)]
    cut = len(steps) // 2
    for h, s in steps[:cut]:
        ring(1, h, s - 1).wait_recv()
        ring(1, h, s).start()

    for d in range(1, n_tp):
        ocopy(d).wait_recv()
    mixer_out = obuf[nmine, :].astype(F32)
    for d in range(1, n_tp):
        mixer_out = mixer_out + orecv[d - 1].astype(F32)
    middle = (tok_ref[...].astype(F32) + mixer_out).astype(BF16)
    mid[...] = middle
    xmine = pl.ds(pl.multiple_of(g_id * tok, tok), tok)
    xall[xmine, :] = rms_norm(middle.astype(F32), fg_ref[...].astype(F32))

    def xcopy(d):
        return pltpu.make_async_remote_copy(
            src_ref=xall.at[xmine],
            dst_ref=xall.at[xmine],
            send_sem=x_s.at[d - 1],
            recv_sem=x_r.at[d - 1],
            device_id=group_peer(d)[1],
            device_id_type=MESH,
        )

    for d in range(1, n_g):
        xcopy(d).start()
    for h, s in steps[cut:]:
        ring(1, h, s - 1).wait_recv()
        ring(1, h, s).start()
    ring(2, 0, 1).start()
    ring(2, 1, 1).start()
    for d in range(1, n_g):
        xcopy(d).wait_recv()
    for h in range(2):
        ring(1, h, n_fs - 1).wait_recv()

    gu = g_ref.shape[1]
    hid = d_ref.shape[1]
    chunk = 2 * tok

    def feed(i, carry):
        rows = pl.ds(pl.multiple_of(i * chunk, chunk), chunk)
        pre = jnp.zeros((chunk, gu), F32)
        for s in range(n_fs):
            pre = pre + jnp.dot(
                xall[rows, pl.ds(columns(s), depth)],
                block(1, s)[...],
                preferred_element_type=F32,
            )
        gate = pre[:, :hid]
        if gu == 2 * hid:
            up = pre[:, hid:]
        else:
            up = pltpu.roll(pre, gu - half, 1)[:, :hid]
        hidden = gate * lax.logistic(gate) * up
        if gu != 2 * hid:
            lane = lax.broadcasted_iota(jnp.int32, hidden.shape, 1)
            hidden = jnp.where(lane < half, hidden, 0.0)
        hbuf[rows, :] = hidden.astype(BF16)
        return carry

    lax.fori_loop(0, n_g // 2, feed, 0)

    def pcols(s, h):
        return pl.ds(pl.multiple_of(columns(s) + h * part, part), part)

    def down(s, h):
        weights = block(2, s)[h * part : (h + 1) * part, :]

        def one(i, carry):
            rows = pl.ds(pl.multiple_of(i * chunk, chunk), chunk)
            pbuf[s, h, rows, :] = contract_last(hbuf[rows, :], weights).astype(BF16)
            return carry

        lax.fori_loop(0, n_g // 2, one, 0)

    def pcopy(s, h, d):
        other, where = group_peer(d)
        return pltpu.make_async_remote_copy(
            src_ref=pbuf.at[s, h, pl.ds(pl.multiple_of(other * tok, tok), tok)],
            dst_ref=prow.at[s, h, d - 1],
            send_sem=p_s.at[s, h, d - 1],
            recv_sem=p_r.at[s, h, d - 1],
            device_id=where,
            device_id_type=MESH,
        )

    for s in range(n_fs):
        for h in range(2):
            if s > 0:
                ring(2, h, s).wait_recv()
                if s < n_fs - 1:
                    ring(2, h, s + 1).start()
            down(s, h)
            for d in range(1, n_g):
                pcopy(s, h, d).start()
    for s in range(n_fs):
        owner = lax.rem(fs - s + n_fs, n_fs)
        for h in range(2):
            for d in range(1, n_g):
                pcopy(s, h, d).wait_recv()
            total = pbuf[s, h, xmine, :].astype(F32)
            for d in range(1, n_g):
                total = total + prow[s, h, d - 1].astype(F32)
            for o in range(n_fs):

                @pl.when(owner == o)
                def _():
                    cols = slice(o * depth + h * part, o * depth + (h + 1) * part)
                    out_ref[:, cols] = (mid[:, cols].astype(F32) + total).astype(BF16)

    for p in range(3):
        for h in range(2):
            for s in range(1, n_fs):
                ring(p, h, s).wait_send()
    for d in range(1, n_tp):
        ncopy(d).wait_send()
        stcopy(d).wait_send()
        ocopy(d).wait_send()
    for d in range(1, n_g):
        xcopy(d).wait_send()
        for s in range(n_fs):
            for h in range(2):
                pcopy(s, h, d).wait_send()


def round_up(n, m):
    return (n + m - 1) // m * m


def pad_last(x, size):
    return jnp.pad(x, [(0, 0)] * (x.ndim - 1) + [(0, size - x.shape[-1])])


def per_device(
    mesh_sizes,
    tokens,
    mix_gain,
    gate_proj,
    value_proj,
    layer_gain,
    layer_shift,
    mix_kernel,
    mix_offset,
    out_proj,
    ffn_gain,
    ffn_gate,
    ffn_up,
    ffn_down,
):
    n_rep, n_fs, n_tp = mesh_sizes
    tok, model = tokens.shape
    depth, lw = gate_proj.shape
    lwp = round_up(lw, 128)
    width = layer_gain.shape[0]
    groups = mix_kernel.shape[0]
    half = ffn_gate.shape[1] // n_rep
    hid = round_up(half, 128)
    first = lax.axis_index("rep") * half
    gate_half, up_half, down_half = (
        lax.dynamic_slice_in_dim(x, first, half, axis=1) for x in (ffn_gate, ffn_up, ffn_down)
    )
    if (2 * half) % 128 == 0 and half % 128 != 0 and 2 * half >= hid and (2 * half) % 256 == 128:
        gu = jnp.concatenate([gate_half, up_half], axis=1)
    else:
        gu = jnp.concatenate([pad_last(gate_half, hid), pad_last(up_half, hid)], axis=1)
    down = pad_last(down_half, hid)
    mixw = jnp.concatenate([pad_last(x, lwp) for x in (gate_proj, value_proj, out_proj)], axis=1)
    lgain = pad_last(layer_gain.astype(F32).reshape(n_tp, 1, lw), lwp)
    lshift = pad_last(layer_shift.astype(F32).reshape(n_tp, 1, lw), lwp)
    offset = mix_offset.astype(F32)[:, :, None]
    n_g = n_rep * n_tp
    guw = gu.shape[1]
    part = depth // 2
    sizes = (n_rep, n_fs, n_tp, width, lw, lwp, width // groups, half)
    vmem = pl.BlockSpec(memory_space=pltpu.VMEM)
    dma = pltpu.SemaphoreType.DMA
    return pl.pallas_call(
        functools.partial(kernel, sizes),
        out_shape=jax.ShapeDtypeStruct((tok, model), BF16),
        in_specs=[vmem] * 10,
        out_specs=vmem,
        scratch_shapes=[
            pltpu.VMEM((n_fs - 1, depth, 3 * lwp), BF16),
            pltpu.VMEM((n_fs - 1, depth, guw), BF16),
            pltpu.VMEM((n_fs - 1, depth, hid), BF16),
            pltpu.VMEM((n_tp * tok, model), BF16),
            pltpu.VMEM((n_tp * tok, lwp), F32),
            pltpu.VMEM((n_tp * tok, lwp), F32),
            pltpu.VMEM((n_tp, n_tp, 8, tok), F32),
            pltpu.VMEM((n_tp * tok, model), BF16),
            pltpu.VMEM((n_tp - 1, tok, model), BF16),
            pltpu.VMEM((tok, model), BF16),
            pltpu.VMEM((n_g * tok, model), BF16),
            pltpu.VMEM((n_g * tok, hid), BF16),
            pltpu.VMEM((n_fs, 2, n_g * tok, part), BF16),
            pltpu.VMEM((n_fs, 2, n_g - 1, tok, part), BF16),
            dma((3, 2, n_fs - 1)),
            dma((3, 2, n_fs - 1)),
            dma((n_tp - 1,)),
            dma((n_tp - 1,)),
            dma((n_tp - 1,)),
            dma((n_tp - 1,)),
            dma((n_tp - 1,)),
            dma((n_tp - 1,)),
            dma((n_g - 1,)),
            dma((n_g - 1,)),
            dma((n_fs, 2, n_g - 1)),
            dma((n_fs, 2, n_g - 1)),
        ],
        compiler_params=pltpu.CompilerParams(
            collective_id=0, has_side_effects=True, vmem_limit_bytes=67043328
        ),
    )(
        tokens,
        mix_gain.reshape(1, -1),
        lgain,
        lshift,
        mix_kernel,
        offset,
        ffn_gain.reshape(1, -1),
        mixw,
        gu,
        down,
    )


def solution(mesh):
    placed = (
        P(("rep", "fs", "tp"), None),
        P(),
        P("fs", "tp"),
        P("fs", "tp"),
        P(),
        P(),
        P(),
        P(),
        P("fs", "tp"),
        P(),
        P("fs", "tp"),
        P("fs", "tp"),
        P("fs", "tp"),
    )
    mesh_sizes = tuple(mesh.shape[a] for a in ("rep", "fs", "tp"))
    return jax.shard_map(
        functools.partial(per_device, mesh_sizes),
        mesh=mesh,
        in_specs=placed,
        out_specs=P(("rep", "fs", "tp"), None),
        check_vma=False,
    )
```

```python
import functools

import jax
import jax.numpy as jnp
from jax import lax
from jax.experimental import pallas as pl
from jax.experimental.pallas import tpu as pltpu
from jax.sharding import PartitionSpec as P

epsilon = 1e-06
MESH = pl.DeviceIdType.MESH
F32 = jnp.float32
BF16 = jnp.bfloat16


def rms_norm(floats, gain):
    scale = lax.rsqrt(jnp.mean(floats * floats, axis=-1, keepdims=True) + epsilon)
    return (floats * scale * gain).astype(BF16)


def gelu(x):
    inner = 0.7978845608028654 * (x + 0.044715 * (x * x * x))
    return 0.5 * x * (1.0 + jnp.tanh(inner))


def contract_last(left, right):
    return lax.dot_general(left, right, (((1,), (1,)), ((), ())), preferred_element_type=F32)


def kernel(
    sizes,
    tok_ref,
    mg_ref,
    lg_ref,
    ls_ref,
    mk_ref,
    mo_ref,
    fg_ref,
    m_ref,
    g_ref,
    d_ref,
    out_ref,
    mbuf,
    gbuf,
    dbuf,
    nall,
    gate_u,
    act,
    stats,
    obuf,
    orecv,
    mid,
    xall,
    hbuf,
    pbuf,
    prow,
    ring_s,
    ring_r,
    e_s,
    e_r,
    n_s,
    n_r,
    st_s,
    st_r,
    o_s,
    o_r,
    x_s,
    x_r,
    p_s,
    p_r,
):
    n_rep, n_fs, n_tp, width, lw, lwp, group_ch, half = sizes
    tok, model = tok_ref.shape
    depth = m_ref.shape[0]
    part = depth // 2
    rep, fs, tp = lax.axis_index("rep"), lax.axis_index("fs"), lax.axis_index("tp")
    n_g = n_rep * n_tp
    g_id = rep * n_tp + tp
    right = lax.rem(fs + 1, n_fs)
    left = lax.rem(fs + n_fs - 1, n_fs)

    def group_peer(d):
        other = lax.rem(g_id + d, n_g)
        return other, {"rep": other // n_tp, "tp": lax.rem(other, n_tp)}

    def tp_peer(d):
        other = lax.rem(tp + d, n_tp)
        return other, {"tp": other}

    barrier = pltpu.get_barrier_semaphore()
    for side in (left, right):
        pl.semaphore_signal(barrier, inc=1, device_id={"fs": side}, device_id_type=MESH)
    for d in range(1, n_g):
        pl.semaphore_signal(barrier, inc=1, device_id=group_peer(d)[1], device_id_type=MESH)
    pl.semaphore_wait(barrier, n_g + 1)

    held = ((m_ref, mbuf), (g_ref, gbuf), (d_ref, dbuf))

    def block(p, s):
        return held[p][0] if s == 0 else held[p][1].at[s - 1]

    share = depth // n_rep
    piece = share // 2

    def mixer_rows(h):
        return pl.ds(pl.multiple_of(rep * share + h * piece, piece), piece)

    def ring(p, h, s):
        size = d_ref.shape[0] // 2 if p == 2 else part
        rows = mixer_rows(h) if p == 0 else pl.ds(h * size, size)
        return pltpu.make_async_remote_copy(
            src_ref=block(p, s - 1).at[rows],
            dst_ref=block(p, s).at[rows],
            send_sem=ring_s.at[p, h, s - 1],
            recv_sem=ring_r.at[p, h, s - 1],
            device_id={"fs": right},
            device_id_type=MESH,
        )

    def across(h, s, e):
        return pltpu.make_async_remote_copy(
            src_ref=mbuf.at[s - 1, mixer_rows(h)],
            dst_ref=mbuf.at[s - 1, mixer_rows(h)],
            send_sem=e_s.at[e - 1, h, s - 1],
            recv_sem=e_r.at[e - 1, h, s - 1],
            device_id={"rep": lax.rem(rep + e, n_rep)},
            device_id_type=MESH,
        )

    def columns(s):
        owner = lax.rem(fs - s + n_fs, n_fs)
        return pl.multiple_of(owner * depth, 128)

    ring(0, 0, 1).start()
    ring(0, 1, 1).start()

    nmine = pl.ds(pl.multiple_of(tp * tok, tok), tok)
    nall[nmine, :] = rms_norm(tok_ref[...].astype(F32), mg_ref[...].astype(F32))

    def ncopy(d):
        return pltpu.make_async_remote_copy(
            src_ref=nall.at[nmine],
            dst_ref=nall.at[nmine],
            send_sem=n_s.at[d - 1],
            recv_sem=n_r.at[d - 1],
            device_id=tp_peer(d)[1],
            device_id_type=MESH,
        )

    for d in range(1, n_tp):
        ncopy(d).start()
    for s in range(1, n_fs):
        for h in range(2):
            ring(0, h, s).wait_recv()
            if s < n_fs - 1:
                ring(0, h, s + 1).start()
                if s == n_fs - 2:
                    ring(1, h, 1).start()
            for e in range(1, n_rep):
                across(h, s, e).start()
    for s in range(1, n_fs):
        for h in range(2):
            for e in range(1, n_rep):
                across(h, s, e).wait_recv()
    for d in range(1, n_tp):
        ncopy(d).wait_recv()

    rows_tp = n_tp * tok

    def project(i, carry):
        rows = pl.ds(pl.multiple_of(i * tok, tok), tok)
        pre = jnp.zeros((tok, 2 * lwp), F32)
        for s in range(n_fs):
            pre = pre + jnp.dot(
                nall[rows, pl.ds(columns(s), depth)],
                block(0, s)[:, : 2 * lwp],
                preferred_element_type=F32,
            )
        gate_u[rows, :] = gelu(pre[:, :lwp])
        a = gelu(pre[:, lwp:])
        act[rows, :] = a
        flipped = a.T
        one = jnp.sum(flipped, axis=0, keepdims=True)
        two = jnp.sum(flipped * flipped, axis=0, keepdims=True)
        which = lax.broadcasted_iota(jnp.int32, (8, tok), 0)
        stats[0, i] = jnp.where(which == 0, one, two)
        return carry

    lax.fori_loop(0, n_tp, project, 0)

    def stcopy(d):
        return pltpu.make_async_remote_copy(
            src_ref=stats.at[0],
            dst_ref=stats.at[d],
            send_sem=st_s.at[d - 1],
            recv_sem=st_r.at[d - 1],
            device_id=tp_peer(d)[1],
            device_id_type=MESH,
        )

    for d in range(1, n_tp):
        stcopy(d).start()
    for d in range(1, n_tp):
        stcopy(d).wait_recv()

    group = (tp * lw) // group_ch
    span = mk_ref.shape[1]
    at_t = lax.broadcasted_iota(jnp.int32, (span, span), 0)
    at_s = lax.broadcasted_iota(jnp.int32, (span, span), 1)
    mix_k = jnp.where(at_s <= at_t, mk_ref[group].astype(F32), 0.0).astype(BF16)
    gain_part, shift_part = lg_ref[tp], ls_ref[tp]
    offsets = mo_ref[...].astype(F32)
    chosen = lax.broadcasted_iota(jnp.int32, offsets.shape, 0) == group
    offset = jnp.sum(jnp.where(chosen, offsets, 0.0), axis=0, keepdims=True)
    offset = jnp.broadcast_to(offset, (span, span)).T[:, 0:1]

    def mix(i, carry):
        rows = pl.ds(pl.multiple_of(i * tok, tok), tok)
        total = stats[0, i]
        for d in range(1, n_tp):
            total = total + stats[d, i]
        flipped = jnp.concatenate([total] * 16, axis=0).T
        center = flipped[:, 0:1] / width
        spread = flipped[:, 1:2] / width - center * center
        values = (
            (act[rows, :] - center) * lax.rsqrt(spread + epsilon) * gain_part + shift_part
        ).astype(BF16)
        gates = gate_u[rows, :]
        for b in range(tok // span):
            cut = slice(b * span, (b + 1) * span)
            mixing = jnp.dot(mix_k, values[cut], preferred_element_type=F32) + offset
            gated = (gates[cut] * mixing).astype(BF16)
            to = pl.ds(pl.multiple_of(i * tok + b * span, span), span)
            for s in range(n_fs):
                obuf[to, pl.ds(columns(s), depth)] = contract_last(
                    gated, block(0, s)[:, 2 * lwp :]
                ).astype(BF16)
        return carry

    lax.fori_loop(0, n_tp, mix, 0)

    def ocopy(d):
        other, where = tp_peer(d)
        return pltpu.make_async_remote_copy(
            src_ref=obuf.at[pl.ds(pl.multiple_of(other * tok, tok), tok)],
            dst_ref=orecv.at[d - 1],
            send_sem=o_s.at[d - 1],
            recv_sem=o_r.at[d - 1],
            device_id=where,
            device_id_type=MESH,
        )

    for d in range(1, n_tp):
        ocopy(d).start()

    steps = [(h, s) for s in range(2, n_fs) for h in range(2)]
    cut = len(steps) // 2
    for h, s in steps[:cut]:
        ring(1, h, s - 1).wait_recv()
        ring(1, h, s).start()

    for d in range(1, n_tp):
        ocopy(d).wait_recv()
    mixer_out = obuf[nmine, :].astype(F32)
    for d in range(1, n_tp):
        mixer_out = mixer_out + orecv[d - 1].astype(F32)
    middle = (tok_ref[...].astype(F32) + mixer_out).astype(BF16)
    mid[...] = middle
    xmine = pl.ds(pl.multiple_of(g_id * tok, tok), tok)
    xall[xmine, :] = rms_norm(middle.astype(F32), fg_ref[...].astype(F32))

    def xcopy(d):
        return pltpu.make_async_remote_copy(
            src_ref=xall.at[xmine],
            dst_ref=xall.at[xmine],
            send_sem=x_s.at[d - 1],
            recv_sem=x_r.at[d - 1],
            device_id=group_peer(d)[1],
            device_id_type=MESH,
        )

    for d in range(1, n_g):
        xcopy(d).start()
    for h, s in steps[cut:]:
        ring(1, h, s - 1).wait_recv()
        ring(1, h, s).start()
    ring(2, 0, 1).start()
    ring(2, 1, 1).start()
    for d in range(1, n_g):
        xcopy(d).wait_recv()
    for h in range(2):
        ring(1, h, n_fs - 1).wait_recv()

    gu = g_ref.shape[1]
    hid = hbuf.shape[1]
    packed = d_ref.shape[1] != hid
    chunk = 2 * tok

    def feed(i, carry):
        rows = pl.ds(pl.multiple_of(i * chunk, chunk), chunk)
        pre = jnp.zeros((chunk, gu), F32)
        for s in range(n_fs):
            pre = pre + jnp.dot(
                xall[rows, pl.ds(columns(s), depth)],
                block(1, s)[...],
                preferred_element_type=F32,
            )
        gate = pre[:, :hid]
        if gu == 2 * hid:
            up = pre[:, hid:]
        else:
            up = pltpu.roll(pre, gu - half, 1)[:, :hid]
        hidden = gate * lax.logistic(gate) * up
        if gu != 2 * hid:
            lane = lax.broadcasted_iota(jnp.int32, hidden.shape, 1)
            hidden = jnp.where(lane < half, hidden, 0.0)
        hbuf[rows, :] = hidden.astype(BF16)
        return carry

    loops = n_g // 2
    lax.fori_loop(0, loops // 2, feed, 0)
    ring(2, 0, 1).wait_recv()
    ring(2, 0, 2).start()
    lax.fori_loop(loops // 2, loops, feed, 0)

    def down(s, h):
        size = d_ref.shape[0] // 2
        weights = block(2, s)[h * size : (h + 1) * size, :]
        if packed:
            turned = pltpu.roll(weights.astype(F32), half, 1).astype(BF16)
            weights = jnp.concatenate([weights[:, :hid], turned[:, :hid]], axis=0)

        def one(i, carry):
            rows = pl.ds(pl.multiple_of(i * chunk, chunk), chunk)
            pbuf[s, h, rows, :] = contract_last(hbuf[rows, :], weights).astype(BF16)
            return carry

        lax.fori_loop(0, n_g // 2, one, 0)

    def pcopy(s, h, d):
        other, where = group_peer(d)
        return pltpu.make_async_remote_copy(
            src_ref=pbuf.at[s, h, pl.ds(pl.multiple_of(other * tok, tok), tok)],
            dst_ref=prow.at[s, h, d - 1],
            send_sem=p_s.at[s, h, d - 1],
            recv_sem=p_r.at[s, h, d - 1],
            device_id=where,
            device_id_type=MESH,
        )

    for s in range(n_fs):
        for h in range(2):
            if s > 0:
                if (h, s) != (0, 1):
                    ring(2, h, s).wait_recv()
                    if s < n_fs - 1:
                        ring(2, h, s + 1).start()
            down(s, h)
            for d in range(1, n_g):
                pcopy(s, h, d).start()
    for s in range(n_fs):
        owner = lax.rem(fs - s + n_fs, n_fs)
        for h in range(2):
            for d in range(1, n_g):
                pcopy(s, h, d).wait_recv()
            total = pbuf[s, h, xmine, :].astype(F32)
            for d in range(1, n_g):
                total = total + prow[s, h, d - 1].astype(F32)
            for o in range(n_fs):

                @pl.when(owner == o)
                def _():
                    cols = slice(o * depth + h * part, o * depth + (h + 1) * part)
                    out_ref[:, cols] = (mid[:, cols].astype(F32) + total).astype(BF16)

    for p in range(3):
        for h in range(2):
            for s in range(1, n_fs):
                ring(p, h, s).wait_send()
                if p == 0:
                    for e in range(1, n_rep):
                        across(h, s, e).wait_send()
    for d in range(1, n_tp):
        ncopy(d).wait_send()
        stcopy(d).wait_send()
        ocopy(d).wait_send()
    for d in range(1, n_g):
        xcopy(d).wait_send()
        for s in range(n_fs):
            for h in range(2):
                pcopy(s, h, d).wait_send()


def round_up(n, m):
    return (n + m - 1) // m * m


def pad_last(x, size):
    return jnp.pad(x, [(0, 0)] * (x.ndim - 1) + [(0, size - x.shape[-1])])


def per_device(
    mesh_sizes,
    tokens,
    mix_gain,
    gate_proj,
    value_proj,
    layer_gain,
    layer_shift,
    mix_kernel,
    mix_offset,
    out_proj,
    ffn_gain,
    ffn_gate,
    ffn_up,
    ffn_down,
):
    n_rep, n_fs, n_tp = mesh_sizes
    tok, model = tokens.shape
    depth, lw = gate_proj.shape
    lwp = round_up(lw, 128)
    width = layer_gain.shape[0]
    groups = mix_kernel.shape[0]
    half = ffn_gate.shape[1] // n_rep
    hid = round_up(half, 128)
    first = lax.axis_index("rep") * half
    gate_half, up_half, down_half = (
        lax.dynamic_slice_in_dim(x, first, half, axis=1) for x in (ffn_gate, ffn_up, ffn_down)
    )
    part = depth // 2
    if half % 128 == 64 and half > 64 and part % 256 == 0:
        gu = jnp.concatenate([gate_half, up_half], axis=1)
        runs = [down_half[i * part // 2 : (i + 1) * part // 2] for i in range(4)]
        down = jnp.concatenate(
            [jnp.concatenate(runs[:2], axis=1), jnp.concatenate(runs[2:], axis=1)], axis=0
        )
    else:
        gu = jnp.concatenate([pad_last(gate_half, hid), pad_last(up_half, hid)], axis=1)
        down = pad_last(down_half, hid)
    mixw = jnp.concatenate([pad_last(x, lwp) for x in (gate_proj, value_proj, out_proj)], axis=1)
    lgain = pad_last(layer_gain.astype(F32).reshape(n_tp, 1, lw), lwp)
    lshift = pad_last(layer_shift.astype(F32).reshape(n_tp, 1, lw), lwp)
    n_g = n_rep * n_tp
    guw = gu.shape[1]
    sizes = (n_rep, n_fs, n_tp, width, lw, lwp, width // groups, half)
    vmem = pl.BlockSpec(memory_space=pltpu.VMEM)
    dma = pltpu.SemaphoreType.DMA
    return pl.pallas_call(
        functools.partial(kernel, sizes),
        out_shape=jax.ShapeDtypeStruct((tok, model), BF16),
        in_specs=[vmem] * 10,
        out_specs=vmem,
        scratch_shapes=[
            pltpu.VMEM((n_fs - 1, depth, 3 * lwp), BF16),
            pltpu.VMEM((n_fs - 1, depth, guw), BF16),
            pltpu.VMEM((n_fs - 1,) + down.shape, BF16),
            pltpu.VMEM((n_tp * tok, model), BF16),
            pltpu.VMEM((n_tp * tok, lwp), F32),
            pltpu.VMEM((n_tp * tok, lwp), F32),
            pltpu.VMEM((n_tp, n_tp, 8, tok), F32),
            pltpu.VMEM((n_tp * tok, model), BF16),
            pltpu.VMEM((n_tp - 1, tok, model), BF16),
            pltpu.VMEM((tok, model), BF16),
            pltpu.VMEM((n_g * tok, model), BF16),
            pltpu.VMEM((n_g * tok, hid), BF16),
            pltpu.VMEM((n_fs, 2, n_g * tok, part), BF16),
            pltpu.VMEM((n_fs, 2, n_g - 1, tok, part), BF16),
            dma((3, 2, n_fs - 1)),
            dma((3, 2, n_fs - 1)),
            dma((n_rep - 1, 2, n_fs - 1)),
            dma((n_rep - 1, 2, n_fs - 1)),
            dma((n_tp - 1,)),
            dma((n_tp - 1,)),
            dma((n_tp - 1,)),
            dma((n_tp - 1,)),
            dma((n_tp - 1,)),
            dma((n_tp - 1,)),
            dma((n_g - 1,)),
            dma((n_g - 1,)),
            dma((n_fs, 2, n_g - 1)),
            dma((n_fs, 2, n_g - 1)),
        ],
        compiler_params=pltpu.CompilerParams(
            collective_id=0, has_side_effects=True, vmem_limit_bytes=67043328
        ),
    )(
        tokens,
        mix_gain.reshape(1, -1),
        lgain,
        lshift,
        mix_kernel,
        mix_offset,
        ffn_gain.reshape(1, -1),
        mixw,
        gu,
        down,
    )


def solution(mesh):
    placed = (
        P(("rep", "fs", "tp"), None),
        P(),
        P("fs", "tp"),
        P("fs", "tp"),
        P(),
        P(),
        P(),
        P(),
        P("fs", "tp"),
        P(),
        P("fs", "tp"),
        P("fs", "tp"),
        P("fs", "tp"),
    )
    mesh_sizes = tuple(mesh.shape[a] for a in ("rep", "fs", "tp"))
    return jax.shard_map(
        functools.partial(per_device, mesh_sizes),
        mesh=mesh,
        in_specs=placed,
        out_specs=P(("rep", "fs", "tp"), None),
        check_vma=False,
    )
```
